32 devices in a mesh: ep: 8 (over z, y), tp: 4 (over x, core).
Axes of the slice: x: 2, y: 2, z: 4, core: 2. Of those that a mesh axis runs over, the one named last changes fastest.
Arguments:
- tokens: bfloat16 [4096, 2048], P(('ep', 'tp')), may hold values from -6 to 6
- norm_gain: float32 [2048], replicated, may hold values from 0.1 to 1.9
- w_gate: bfloat16 [32, 2048, 512], P(('ep', 'tp')), may hold values from -0.125 to 0.125
- w_up: bfloat16 [32, 2048, 512], P(('ep', 'tp')), may hold values from -0.125 to 0.125
- w_down: bfloat16 [32, 512, 2048], P(('ep', 'tp')), may hold values from -0.25 to 0.25
- routing: int32 [4096, 2], P(('ep', 'tp')), may hold values from 0 to 31, as said below
- gate_weight: float32 [4096, 2], P(('ep', 'tp')), may hold values from 0.05 to 1
Outputs:
- combined: bfloat16 [4096, 2048], P(('ep', 'tp'))
The draws below stay inside these ranges and needn't reach their ends.
Inputs may be any that keep to these rules, and one draw needn't show every extreme that they name: `routing`: A token's 2 experts are distinct and lie in one group of 4 consecutive experts. Of the 128 tokens of each device exactly 16 choose each group; no expert is named by more than 16 tokens of one device, and in every group one expert is named by exactly 16 tokens of every device.
All inputs are finite; a program needn't handle non-finite values.
Results may differ from the reference program's by a relative error of at most 0.0085.
Values may be sent and summed in bfloat16 or wider, within the bound.
A program may use at most 64 MiB of HBM per device.

```python
import math
import jax
import jax.numpy as jnp
from jax import lax

D = 2048
FF = 512
GROUP_EXPERTS = 4
TOP = 2
TOK_DEV = 128
EXPERTS = 32
GROUPS = 8
CAP = 16
TOKENS = 4096


def draw_routing(key, part):
    source_count = TOKENS // TOK_DEV
    heavy_key = jax.random.fold_in(key, 11)
    cut_key = jax.random.fold_in(key, 12)
    shuffle_key = jax.random.fold_in(key, 13)
    heavy_member = jax.random.randint(heavy_key, (GROUPS,), 0, GROUP_EXPERTS)
    cut_points = jax.random.randint(cut_key, (source_count, GROUPS, 2), 0, CAP + 1)
    lower = jnp.min(cut_points, axis=-1)
    higher = jnp.max(cut_points, axis=-1)
    rest_loads = jnp.stack([lower, higher - lower, CAP - higher], axis=-1)
    members = jnp.arange(GROUP_EXPERTS, dtype=jnp.int32)
    is_heavy = members[None, :] == heavy_member[:, None]
    rank = jnp.clip(members[None, :] - (members[None, :] > heavy_member[:, None]).astype(jnp.int32), 0, 2)
    rank_full = jnp.broadcast_to(rank[None], (source_count, GROUPS, GROUP_EXPERTS))
    load_table = jnp.where(is_heavy[None], CAP, jnp.take_along_axis(rest_loads, rank_full, axis=2))
    bounds = jnp.cumsum(load_table, axis=-1)
    entries = jnp.arange(2 * CAP, dtype=jnp.int32)
    local_ident = jnp.sum((entries[None, None, :, None] >= bounds[:, :, None, :GROUP_EXPERTS - 1]).astype(jnp.int32), axis=-1)
    group_base = jnp.arange(GROUPS, dtype=jnp.int32) * GROUP_EXPERTS
    pair_table = jnp.stack([local_ident[:, :, :CAP], local_ident[:, :, CAP:]], axis=-1) + group_base[None, :, None, None]
    pair_table = pair_table.reshape(source_count, TOK_DEV, TOP)
    shuffles = jax.vmap(lambda subkey: jax.random.permutation(subkey, TOK_DEV))(jax.random.split(shuffle_key, source_count))
    routing = jnp.take_along_axis(pair_table, shuffles[:, :, None].astype(jnp.int32), axis=1)
    return routing.reshape(TOKENS, TOP).astype(jnp.int32)


def level_of(rng, shape, shards, low, top_value):
    level, own = 1.0, jax.random.fold_in(rng, 6)
    for dim, blocks in shards:
        steps = jnp.exp(jax.random.uniform(jax.random.fold_in(own, dim), (blocks,), jnp.float32, low / len(shards), top_value / len(shards)))
        level = level * jnp.repeat(steps, shape[dim] // blocks).reshape([-1 if axis == dim else 1 for axis in range(len(shape))])
    return level


def gaussian(rng, shape, spread, most, cuts=(), kind=jnp.bfloat16):
    values = spread * jax.random.normal(rng, shape, jnp.float32)
    if cuts:
        values = values * level_of(rng, shape, cuts, -0.22, 0.18)
    return jnp.clip(values, -most, most).astype(kind)


def setup_inputs(seed: int = 0) -> dict:
    key_list = jax.random.split(jax.random.key(seed), 8)
    tokens = gaussian(key_list[0], (TOKENS, D), 1.0, 6.0, ((0, 32),))
    norm_gain = jnp.clip(1.0 + 0.18 * jax.random.normal(key_list[1], (D,), jnp.float32), 0.1, 1.9)
    w_gate = gaussian(key_list[2], (EXPERTS, D, FF), D ** -0.5, 0.125, ((0, 32),))
    w_up = gaussian(key_list[3], (EXPERTS, D, FF), D ** -0.5, 0.125, ((0, 32),))
    w_down = gaussian(key_list[4], (EXPERTS, FF, D), FF ** -0.5, 0.25, ((0, 32),))
    routing = draw_routing(jax.random.fold_in(key_list[7], 71), 0)
    gate_weight = jnp.clip(jnp.exp(math.log(1.0) - 2.9957323 * jax.random.uniform(key_list[6], (TOKENS, TOP), jnp.float32) ** level_of(key_list[6], (TOKENS, TOP), ((0, 32),), -0.2, 0.2)), 0.05, 1.0)
    return {"tokens": tokens, "norm_gain": norm_gain, "w_gate": w_gate, "w_up": w_up, "w_down": w_down, "routing": routing, "gate_weight": gate_weight}


def reference(tokens, norm_gain, w_gate, w_up, w_down, routing, gate_weight):
    source_count = TOKENS // TOK_DEV
    values = tokens.astype(jnp.float32)
    scale = lax.rsqrt(lax.optimization_barrier(jnp.mean(values * values, axis=-1, keepdims=True)) + 1e-06)
    normed = (values * scale * norm_gain.astype(jnp.float32)).astype(jnp.bfloat16)
    assigned = routing.reshape(source_count, TOK_DEV * TOP).astype(jnp.int32)

    def count_slots(block):
        onehot = (block[:, None] == jnp.arange(EXPERTS, dtype=jnp.int32)[None, :]).astype(jnp.int32)
        running = jnp.cumsum(onehot, axis=0)
        return lax.optimization_barrier(jnp.sum(onehot * running, axis=1)) - 1
    slot_index = lax.map(count_slots, assigned)
    source_index = jnp.arange(source_count, dtype=jnp.int32)[:, None]
    position = (assigned * source_count + source_index) * CAP + slot_index
    dump_index = TOKENS * TOP
    slot_owner = jnp.full((EXPERTS * source_count * CAP,), dump_index, jnp.int32)
    slot_owner = slot_owner.at[position.reshape(-1)].set(jnp.arange(TOKENS * TOP, dtype=jnp.int32))
    slot_owner = slot_owner.reshape(EXPERTS, source_count * CAP)
    normed_pad = jnp.concatenate([normed, jnp.zeros((1, D), jnp.bfloat16)], axis=0)

    def one_expert(expert, results):
        owners = lax.dynamic_index_in_dim(slot_owner, expert, 0, keepdims=False)
        slot_rows = normed_pad[owners // TOP]
        gate_part = jnp.dot(slot_rows, lax.dynamic_index_in_dim(w_gate, expert, 0, keepdims=False), preferred_element_type=jnp.float32)
        up_part = jnp.dot(slot_rows, lax.dynamic_index_in_dim(w_up, expert, 0, keepdims=False), preferred_element_type=jnp.float32)
        hidden = (jax.nn.silu(gate_part) * up_part).astype(jnp.bfloat16)
        expert_out = jnp.dot(hidden, lax.dynamic_index_in_dim(w_down, expert, 0, keepdims=False), preferred_element_type=jnp.float32).astype(jnp.bfloat16)
        return results.at[owners].set(expert_out)
    results = lax.fori_loop(0, EXPERTS, one_expert, jnp.zeros((TOKENS * TOP + 1, D), jnp.bfloat16))
    picked = results[:TOKENS * TOP].reshape(TOKENS, TOP, D).astype(jnp.float32)
    return lax.optimization_barrier(jnp.sum(gate_weight.astype(jnp.float32)[:, :, None] * picked, axis=1)).astype(jnp.bfloat16)
```

```python
import functools
import jax
import jax.numpy as jnp
from jax import lax
from jax.experimental import pallas as pl
from jax.experimental.pallas import tpu as pltpu
from jax.sharding import PartitionSpec as P

BF = jnp.bfloat16
F32 = jnp.float32
MESH = pl.DeviceIdType.MESH


def flip(index, bits):
    unit = 1
    while unit <= bits:
        if bits & unit:
            index = index + unit - 2 * unit * lax.rem(lax.div(index, unit), 2)
        unit *= 2
    return index


def kernel(
    ep_count, tp_count, block, chunks,
    tok_ref, gain_ref, route_ref, gate_ref, wg_hbm, wu_hbm, wd_hbm, out_ref,
    wg, wu, wd, xcat, pack, rows_in, hid, part, pair_in, cross_out, cross_in, done, back,
    w_sem, disp_s, disp_r, core_s, core_r, x_s, x_r, fwd_s, fwd_r,
    pair_s, pair_r, cross_s, cross_r, ret_s, ret_r,
):
    toks, width = tok_ref.shape
    ff = wg.shape[1]
    slots = ep_count * block
    per = ep_count // chunks
    seg = per * block
    me_e = lax.axis_index("ep")
    me_t = lax.axis_index("tp")
    partner = {"tp": flip(me_t, 1)}
    across = {"tp": flip(me_t, 2)}
    peer = [{"ep": flip(me_e, d)} for d in range(ep_count)]

    w_copies = [
        pltpu.make_async_copy(src.at[0], dst, w_sem.at[i])
        for i, (src, dst) in enumerate(((wg_hbm, wg), (wu_hbm, wu), (wd_hbm, wd)))
    ]
    for c in w_copies:
        c.start()
    barrier = pltpu.get_barrier_semaphore()
    others = peer[1:] + [partner, across]
    for dev in others:
        pl.semaphore_signal(barrier, inc=1, device_id=dev, device_id_type=MESH)

    values = tok_ref[...].astype(F32)
    scale = lax.rsqrt(jnp.mean(values * values, axis=-1, keepdims=True) + 1e-06)
    xcat[:, :width] = (values * scale * gain_ref[...]).astype(BF)
    lane = lax.broadcasted_iota(jnp.int32, (toks, 128), 1)
    weight = jnp.zeros((toks, 128), F32)
    for k in range(route_ref.shape[1]):
        member = jnp.bitwise_and(route_ref[:, k : k + 1], tp_count - 1)
        hit = member == jnp.bitwise_and(lane, tp_count - 1)
        weight = weight + jnp.where(hit, gate_ref[:, k : k + 1], 0.0)
    hi = weight.astype(BF).astype(F32)
    mid = (weight - hi).astype(BF).astype(F32)
    low = weight - hi - mid
    tail = jnp.where(lane < tp_count, hi, jnp.where(lane < 2 * tp_count, mid, low))
    xcat[:, width:] = jnp.where(lane < 3 * tp_count, tail, 0.0).astype(BF)

    shift = tp_count.bit_length() - 1
    group = jnp.bitwise_xor(jnp.right_shift(route_ref[:, 0:1], shift), me_e)
    in_group = (group == lane).astype(F32)
    below = lax.broadcasted_iota(jnp.int32, (toks, toks), 0) > lax.broadcasted_iota(
        jnp.int32, (toks, toks), 1
    )
    ranks = jnp.dot(
        below.astype(F32).astype(BF), in_group.astype(BF), preferred_element_type=F32
    )
    rank = jnp.sum(ranks * in_group, axis=-1, keepdims=True).astype(jnp.int32)
    slot = group * block + rank
    slot_lane = lax.broadcasted_iota(jnp.int32, (toks, slots), 1)
    unpack = (slot == slot_lane).astype(F32)
    packing = unpack.T.astype(BF)
    step = min(slots, 128)
    for s in range(0, slots, step):
        pack[s : s + step, :] = jnp.dot(
            packing[s : s + step, :], xcat[...], preferred_element_type=F32
        ).astype(BF)
    rows_in[0, 0:block, :] = pack[0:block, :]

    pl.semaphore_wait(barrier, len(others))

    def remote(src, dst, s, r, dev):
        return pltpu.make_async_remote_copy(
            src_ref=src, dst_ref=dst, send_sem=s, recv_sem=r, device_id=dev, device_id_type=MESH
        )

    def place(d, pos):
        k, dd = d // per, d % per
        return rows_in.at[k, pl.ds(pos * seg + dd * block, block)]

    disp, core, xs, fwd, ret, pair, cross = {}, {}, {}, {}, {}, {}, {}
    for d in range(1, ep_count):
        disp[d] = remote(
            pack.at[pl.ds(d * block, block)], place(d, 0), disp_s.at[d], disp_r.at[d], peer[d]
        )
        disp[d].start()

    def spread(d):
        if d:
            disp[d].wait_recv()
        xs[d] = remote(place(d, 0), place(d, 1), x_s.at[d], x_r.at[d], across)
        xs[d].start()
        core[d] = remote(place(d, 0), place(d, 2), core_s.at[d], core_r.at[d], partner)
        core[d].start()

    def forward(d):
        xs[d].wait_recv()
        fwd[d] = remote(place(d, 1), place(d, 3), fwd_s.at[d], fwd_r.at[d], partner)
        fwd[d].start()

    def compute(k):
        for d in range(k * per, k * per + per):
            core[d].wait_recv()
            fwd[d].wait_recv()
        if k == 0:
            for c in w_copies:
                c.wait()
        total = tp_count * seg
        ends = lax.broadcasted_iota(jnp.int32, (total, 128), 1)
        mine = jnp.bitwise_and(ends, tp_count - 1) == me_t
        gates = jnp.sum(
            jnp.where(mine, rows_in[k, :, width:].astype(F32), 0.0), axis=-1, keepdims=True
        )
        f_tile = min(ff, 256)

        def up(j, carry):
            cols = pl.ds(pl.multiple_of(j * f_tile, f_tile), f_tile)
            rows = rows_in[k, :, :width]
            g = jnp.dot(rows, wg[:, cols], preferred_element_type=F32)
            u = jnp.dot(rows, wu[:, cols], preferred_element_type=F32)
            hid[:, cols] = (g / (1.0 + jnp.exp(-g)) * u).astype(BF)
            return carry

        lax.fori_loop(0, ff // f_tile, up, 0)
        d_tile = min(width, 512)

        def down(j, carry):
            cols = pl.ds(pl.multiple_of(j * d_tile, d_tile), d_tile)
            y = jnp.dot(hid[...], wd[:, cols], preferred_element_type=F32)
            part[k, :, cols] = (y * gates).astype(BF)
            return carry

        lax.fori_loop(0, width // d_tile, down, 0)
        pair[k] = remote(
            part.at[k, pl.ds(2 * seg, 2 * seg)], pair_in.at[k], pair_s.at[k], pair_r.at[k], partner
        )
        pair[k].start()

    def join_pair(k):
        pair[k].wait_recv()
        cross_out[k] = (
            part[k, seg : 2 * seg, :].astype(F32) + pair_in[k, seg:, :].astype(F32)
        ).astype(BF)
        cross[k] = remote(cross_out.at[k], cross_in.at[k], cross_s.at[k], cross_r.at[k], across)
        cross[k].start()

    def give_back(k):
        cross[k].wait_recv()
        done[k] = (
            part[k, 0:seg, :].astype(F32)
            + pair_in[k, 0:seg, :].astype(F32)
            + cross_in[k].astype(F32)
        ).astype(BF)
        for dd in range(per):
            d = k * per + dd
            if d == 0:
                back[0:block, :] = done[0, 0:block, :]
            else:
                ret[d] = remote(
                    done.at[k, pl.ds(dd * block, block)], back.at[pl.ds(d * block, block)],
                    ret_s.at[d], ret_r.at[d], peer[d],
                )
                ret[d].start()

    def each(f, k, lo=0, hi=None):
        for d in range(k * per + lo, k * per + (per if hi is None else hi)):
            f(d)

    half = per // 2
    each(spread, 0)
    each(forward, 0)
    each(spread, 1)
    compute(0)
    each(forward, 1)
    join_pair(0)
    compute(1)
    give_back(0)
    each(spread, 2)
    join_pair(1)
    each(forward, 2)
    give_back(1)
    compute(2)
    each(spread, 3, 0, half)
    join_pair(2)
    each(spread, 3, half)
    give_back(2)
    each(forward, 3)
    compute(3)
    join_pair(3)
    give_back(3)

    for d in range(1, ep_count):
        ret[d].wait_recv()
    out_ref[...] = jnp.dot(unpack.astype(BF), back[...], preferred_element_type=F32).astype(BF)
    for group_of in (disp, core, xs, fwd, pair, cross, ret):
        for c in group_of.values():
            c.wait_send()


def local(tokens, norm_gain, w_gate, w_up, w_down, routing, gate_weight):
    toks, width = tokens.shape
    ff = w_gate.shape[2]
    ep_count = lax.axis_size("ep")
    tp_count = lax.axis_size("tp")
    assert tp_count == 4 and ep_count % 8 == 0
    cap = toks // ep_count
    block = -(-cap // 16) * 16
    chunks = 4
    slots = ep_count * block
    seg = slots // chunks
    wide = width + 128
    vm = pl.BlockSpec(memory_space=pltpu.VMEM)
    hbm = pl.BlockSpec(memory_space=pl.ANY)
    dma = pltpu.SemaphoreType.DMA
    n_sem = [3] + [ep_count] * 8 + [chunks] * 4 + [ep_count] * 2
    return pl.pallas_call(
        functools.partial(kernel, ep_count, tp_count, block, chunks),
        out_shape=jax.ShapeDtypeStruct((toks, width), BF),
        in_specs=[vm] * 4 + [hbm] * 3,
        out_specs=vm,
        scratch_shapes=[
            pltpu.VMEM((width, ff), BF),
            pltpu.VMEM((width, ff), BF),
            pltpu.VMEM((ff, width), BF),
            pltpu.VMEM((toks, wide), BF),
            pltpu.VMEM((slots, wide), BF),
            pltpu.VMEM((chunks, tp_count * seg, wide), BF),
            pltpu.VMEM((tp_count * seg, ff), BF),
            pltpu.VMEM((chunks, tp_count * seg, width), BF),
            pltpu.VMEM((chunks, 2 * seg, width), BF),
            pltpu.VMEM((chunks, seg, width), BF),
            pltpu.VMEM((chunks, seg, width), BF),
            pltpu.VMEM((chunks, seg, width), BF),
            pltpu.VMEM((slots, width), BF),
        ] + [dma((n,)) for n in n_sem],
        compiler_params=pltpu.CompilerParams(
            collective_id=0, has_side_effects=True, vmem_limit_bytes=60 * 1024 * 1024
        ),
    )(tokens, norm_gain.reshape(1, width), routing, gate_weight, w_gate, w_up, w_down)


def solution(mesh):
    placed = (
        P(("ep", "tp"), None),
        P(),
        P(("ep", "tp"), None, None),
        P(("ep", "tp"), None, None),
        P(("ep", "tp"), None, None),
        P(("ep", "tp"), None),
        P(("ep", "tp"), None),
    )
    return jax.shard_map(
        local, mesh=mesh, in_specs=placed, out_specs=P(("ep", "tp"), None), check_vma=False
    )
```

```python
import functools
import jax
import jax.numpy as jnp
from jax import lax
from jax.experimental import pallas as pl
from jax.experimental.pallas import tpu as pltpu
from jax.sharding import PartitionSpec as P

BF = jnp.bfloat16
F32 = jnp.float32
MESH = pl.DeviceIdType.MESH

SENT = (0, 1, 4, 2, 5, 3, 6, 7)
CUTS = (0, 2, 4, 6, 7, 8)
ORDER = "s0 s1 s2 s3 f0 f1 c0 s4 f2 f3 j0 c1 s5 j1 f4 g0 s6 f5 c2 s7 g1 j2 f6 c3 g2 f7 j3 c4 j4 g3 g4"


def flip(index, bits):
    unit = 1
    while unit <= bits:
        if bits & unit:
            index = index + unit - 2 * unit * lax.rem(lax.div(index, unit), 2)
        unit *= 2
    return index


def kernel(
    ep_count, tp_count, block, cuts,
    tok_ref, gain_ref, route_ref, gate_ref, wg_hbm, wu_hbm, wd_hbm, out_ref,
    wg, wu, wd, xcat, pack, rows_in, hid, part, pair_in, cross_out, cross_in, done, back,
    w_sem, disp_s, disp_r, core_s, core_r, x_s, x_r, fwd_s, fwd_r,
    pair_s, pair_r, cross_s, cross_r, ret_s, ret_r,
):
    toks, width = tok_ref.shape
    ff = wg.shape[1]
    slots = ep_count * block
    chunk_of = {}
    for k in range(len(cuts) - 1):
        for d in range(cuts[k], cuts[k + 1]):
            chunk_of[d] = k
    me_e = lax.axis_index("ep")
    me_t = lax.axis_index("tp")
    partner = {"tp": flip(me_t, 1)}
    across = {"tp": flip(me_t, 2)}
    peer = [{"ep": flip(me_e, d)} for d in range(ep_count)]

    w_copies = [
        pltpu.make_async_copy(src.at[0], dst, w_sem.at[i])
        for i, (src, dst) in enumerate(((wg_hbm, wg), (wu_hbm, wu), (wd_hbm, wd)))
    ]
    for c in w_copies:
        c.start()
    barrier = pltpu.get_barrier_semaphore()
    others = peer[1:] + [partner, across]
    for dev in others:
        pl.semaphore_signal(barrier, inc=1, device_id=dev, device_id_type=MESH)

    shift = tp_count.bit_length() - 1
    group = jnp.bitwise_xor(jnp.right_shift(route_ref[0:1, :], shift), me_e)
    heads = -(-ep_count // 16) * 16
    in_group = (lax.broadcasted_iota(jnp.int32, (heads, toks), 0) == group).astype(F32)
    above = lax.broadcasted_iota(jnp.int32, (toks, toks), 0) < lax.broadcasted_iota(
        jnp.int32, (toks, toks), 1
    )
    ranks = jnp.dot(
        in_group.astype(BF), above.astype(F32).astype(BF), preferred_element_type=F32
    )
    rank = jnp.sum(ranks * in_group, axis=0, keepdims=True).astype(jnp.int32)
    slot = group * block + rank
    packing = (lax.broadcasted_iota(jnp.int32, (slots, toks), 0) == slot).astype(F32)

    line = lax.broadcasted_iota(jnp.int32, (128, toks), 0)
    weight = jnp.zeros((128, toks), F32)
    for k in range(route_ref.shape[0]):
        member = jnp.bitwise_and(route_ref[k : k + 1, :], tp_count - 1)
        hit = jnp.bitwise_and(line, tp_count - 1) == member
        weight = weight + jnp.where(hit, gate_ref[k : k + 1, :], 0.0)
    hi = weight.astype(BF).astype(F32)
    mid = (weight - hi).astype(BF).astype(F32)
    low = weight - hi - mid
    tail = jnp.where(line < tp_count, hi, jnp.where(line < 2 * tp_count, mid, low))
    xcat[:, width:] = jnp.where(line < 3 * tp_count, tail, 0.0).T.astype(BF)
    values = tok_ref[...].astype(F32)
    scale = lax.rsqrt(jnp.mean(values * values, axis=-1, keepdims=True) + 1e-06)
    xcat[:, :width] = (values * scale * gain_ref[...]).astype(BF)
    step = min(slots, 128)
    for s in range(0, slots, step):
        pack[s : s + step, :] = jnp.dot(
            packing[s : s + step, :].astype(BF), xcat[...], preferred_element_type=F32
        ).astype(BF)
    rows_in[0:block, :] = pack[0:block, :]

    pl.semaphore_wait(barrier, len(others))

    def remote(src, dst, s, r, dev):
        return pltpu.make_async_remote_copy(
            src_ref=src, dst_ref=dst, send_sem=s, recv_sem=r, device_id=dev, device_id_type=MESH
        )

    def span(k):
        return cuts[k] * block, (cuts[k + 1] - cuts[k]) * block

    def place(d, pos):
        base, seg = span(chunk_of[d])
        return rows_in.at[pl.ds(4 * base + pos * seg + d * block - base, block)]

    disp, core, xs, fwd, ret, pair, cross = {}, {}, {}, {}, {}, {}, {}
    unit = ep_count // 8
    sent = [n * unit + i for n in SENT for i in range(unit)]
    for d in [d for d in sent if d]:
        disp[d] = remote(
            pack.at[pl.ds(d * block, block)], place(d, 0), disp_s.at[d], disp_r.at[d], peer[d]
        )
        disp[d].start()

    def spread(d):
        if d:
            disp[d].wait_recv()
        xs[d] = remote(place(d, 0), place(d, 1), x_s.at[d], x_r.at[d], across)
        xs[d].start()
        core[d] = remote(place(d, 0), place(d, 2), core_s.at[d], core_r.at[d], partner)
        core[d].start()

    def forward(d):
        xs[d].wait_recv()
        fwd[d] = remote(place(d, 1), place(d, 3), fwd_s.at[d], fwd_r.at[d], partner)
        fwd[d].start()

    def compute(k):
        for d in range(cuts[k], cuts[k + 1]):
            core[d].wait_recv()
            fwd[d].wait_recv()
        if k == first:
            for c in w_copies:
                c.wait()
        base, seg = span(k)
        total = tp_count * seg
        start = tp_count * base
        ends = lax.broadcasted_iota(jnp.int32, (total, 128), 1)
        mine = jnp.bitwise_and(ends, tp_count - 1) == me_t
        gates = jnp.sum(
            jnp.where(mine, rows_in[start : start + total, width:].astype(F32), 0.0),
            axis=-1, keepdims=True,
        )
        f_tile = min(ff, 256)

        def up(j, carry):
            cols = pl.ds(pl.multiple_of(j * f_tile, f_tile), f_tile)
            rows = rows_in[start : start + total, :width]
            g = jnp.dot(rows, wg[:, cols], preferred_element_type=F32)
            u = jnp.dot(rows, wu[:, cols], preferred_element_type=F32)
            hid[:total, cols] = (g / (1.0 + jnp.exp(-g)) * u).astype(BF)
            return carry

        lax.fori_loop(0, ff // f_tile, up, 0)
        d_tile = min(width, 512)

        def down(j, carry):
            cols = pl.ds(pl.multiple_of(j * d_tile, d_tile), d_tile)
            y = jnp.dot(hid[:total, :], wd[:, cols], preferred_element_type=F32)
            part[start : start + total, cols] = (y * gates).astype(BF)
            return carry

        lax.fori_loop(0, width // d_tile, down, 0)
        pair[k] = remote(
            part.at[pl.ds(start + 2 * seg, 2 * seg)], pair_in.at[pl.ds(2 * base, 2 * seg)],
            pair_s.at[k], pair_r.at[k], partner,
        )
        pair[k].start()

    def join_pair(k):
        base, seg = span(k)
        start = tp_count * base
        pair[k].wait_recv()
        cross_out[base : base + seg, :] = (
            part[start + seg : start + 2 * seg, :].astype(F32)
            + pair_in[2 * base + seg : 2 * base + 2 * seg, :].astype(F32)
        ).astype(BF)
        cross[k] = remote(
            cross_out.at[pl.ds(base, seg)], cross_in.at[pl.ds(base, seg)],
            cross_s.at[k], cross_r.at[k], across,
        )
        cross[k].start()

    def give_back(k):
        base, seg = span(k)
        start = tp_count * base
        cross[k].wait_recv()
        done[base : base + seg, :] = (
            part[start : start + seg, :].astype(F32)
            + pair_in[2 * base : 2 * base + seg, :].astype(F32)
            + cross_in[base : base + seg, :].astype(F32)
        ).astype(BF)
        for d in range(cuts[k], cuts[k + 1]):
            if d == 0:
                back[0:block, :] = done[0:block, :]
            else:
                at = pl.ds(d * block, block)
                ret[d] = remote(done.at[at], back.at[at], ret_s.at[d], ret_r.at[d], peer[d])
                ret[d].start()

    steps = ORDER.split()
    first = int(next(s for s in steps if s[0] == "c")[1:])
    for name in steps:
        number = int(name[1:])
        if name[0] in "sf":
            for d in range(number * unit, number * unit + unit):
                (spread if name[0] == "s" else forward)(d)
        else:
            {"c": compute, "j": join_pair, "g": give_back}[name[0]](number)

    for d in range(1, ep_count):
        ret[d].wait_recv()
    out_ref[...] = jnp.dot(packing.T.astype(BF), back[...], preferred_element_type=F32).astype(BF)
    for group_of in (disp, core, xs, fwd, pair, cross, ret):
        for c in group_of.values():
            c.wait_send()


def local(tokens, norm_gain, w_gate, w_up, w_down, routing, gate_weight):
    toks, width = tokens.shape
    ff = w_gate.shape[2]
    ep_count = lax.axis_size("ep")
    tp_count = lax.axis_size("tp")
    assert tp_count == 4 and ep_count % 8 == 0
    cap = toks // ep_count
    block = -(-cap // 16) * 16
    cuts = [c * (ep_count // 8) for c in CUTS]
    chunks = len(cuts) - 1
    slots = ep_count * block
    most = max(b - a for a, b in zip(cuts, cuts[1:])) * block * tp_count
    wide = width + 128
    vm = pl.BlockSpec(memory_space=pltpu.VMEM)
    hbm = pl.BlockSpec(memory_space=pl.ANY)
    dma = pltpu.SemaphoreType.DMA
    n_sem = [3] + [ep_count] * 8 + [chunks] * 4 + [ep_count] * 2
    return pl.pallas_call(
        functools.partial(kernel, ep_count, tp_count, block, cuts),
        out_shape=jax.ShapeDtypeStruct((toks, width), BF),
        in_specs=[vm] * 4 + [hbm] * 3,
        out_specs=vm,
        scratch_shapes=[
            pltpu.VMEM((width, ff), BF),
            pltpu.VMEM((width, ff), BF),
            pltpu.VMEM((ff, width), BF),
            pltpu.VMEM((toks, wide), BF),
            pltpu.VMEM((slots, wide), BF),
            pltpu.VMEM((tp_count * slots, wide), BF),
            pltpu.VMEM((most, ff), BF),
            pltpu.VMEM((tp_count * slots, width), BF),
            pltpu.VMEM((2 * slots, width), BF),
            pltpu.VMEM((slots, width), BF),
            pltpu.VMEM((slots, width), BF),
            pltpu.VMEM((slots, width), BF),
            pltpu.VMEM((slots, width), BF),
        ] + [dma((n,)) for n in n_sem],
        compiler_params=pltpu.CompilerParams(
            collective_id=0, has_side_effects=True, vmem_limit_bytes=60 * 1024 * 1024
        ),
    )(tokens, norm_gain.reshape(1, width), routing.T, gate_weight.T, w_gate, w_up, w_down)


def solution(mesh):
    placed = (
        P(("ep", "tp"), None),
        P(),
        P(("ep", "tp"), None, None),
        P(("ep", "tp"), None, None),
        P(("ep", "tp"), None, None),
        P(("ep", "tp"), None),
        P(("ep", "tp"), None),
    )
    return jax.shard_map(
        local, mesh=mesh, in_specs=placed, out_specs=P(("ep", "tp"), None), check_vma=False
    )
```
